32 devices in a mesh: sp: 8 (over z, y), tp: 4 (over x, core).
Axes of the slice: x: 2, y: 2, z: 4, core: 2. Of those that a mesh axis runs over, the one named last changes fastest.
Arguments:
- stream: bfloat16 [2048, 2048], P(('sp', 'tp')), may hold values from -6 to 6
- queries: bfloat16 [2048, 2048], P('sp', 'tp'), may hold values from -147.07821 to 147.07821
- keys: bfloat16 [2048, 2048], P('sp', 'tp'), may hold values from -7 to 7
- values: bfloat16 [2048, 2048], P('sp', 'tp'), may hold values from -6 to 6
- head_lambda: float32 [8], P('tp'), may hold values from 0.3 to 0.8
- head_gain: float32 [256], replicated, may hold values from 0.1 to 1.9
- w_out: bfloat16 [2048, 2048], P('tp'), may hold values from -0.125 to 0.125
- norm_gain: float32 [2048], replicated, may hold values from 0.1 to 1.9
- w_gate: bfloat16 [2048, 5632], P('sp', 'tp'), may hold values from -0.125 to 0.125
- w_up: bfloat16 [2048, 5632], P('sp', 'tp'), may hold values from -0.125 to 0.125
- w_down: bfloat16 [5632, 2048], P('tp', 'sp'), may hold values from -0.078125 to 0.078125
Outputs:
- result: bfloat16 [2048, 2048], P(('sp', 'tp'))
The draws below stay inside these ranges and needn't reach their ends.
All inputs are finite; a program needn't handle non-finite values.
Results may differ from the reference program's by a relative error of at most 0.013.
Values may be sent and summed in bfloat16 or wider, within the bound.
A program may use at most 192 MiB of HBM per device.

```python
import math
import jax
import jax.numpy as jnp
from jax import lax

D = 2048
H = 8
DH = 128
DV = 256
FF = 5632
TOKENS = 2048


def paired_draw(key):
    base_keys = jnp.clip(jax.random.normal(jax.random.fold_in(key, 11), (TOKENS, 2 * H * DH), jnp.float32), -6.0, 6.0)
    base_queries = 1.7 * jnp.clip(jax.random.normal(jax.random.fold_in(key, 12), (TOKENS, 2 * H * DH), jnp.float32), -6.0, 6.0)
    key_out = base_keys
    query_out = base_queries
    return (query_out, key_out)


def draw_queries(key, part):
    return paired_draw(key)[0].astype(jnp.bfloat16)


def draw_keys(key, part):
    return paired_draw(key)[1].astype(jnp.bfloat16)


def levels(own_key, extent, shards, smallest, largest):
    def one(dim, parts):
        draws = jax.random.uniform(jax.random.fold_in(jax.random.fold_in(own_key, 6), dim), (parts,), jnp.float32, smallest / len(shards), largest / len(shards))
        return jnp.repeat(jnp.exp(draws), extent[dim] // parts).reshape((-1,) + (1,) * (len(extent) - dim - 1))

    factor_of = one(*shards[0])
    for cut in shards[1:]:
        factor_of = factor_of * one(*cut)
    return factor_of


def scatter_about(key, shape, spread, limit, cuts=(), kind=jnp.bfloat16):
    entries = spread * jax.random.normal(key, shape, jnp.float32)
    if cuts:
        entries = entries * levels(key, shape, cuts, -0.22, 0.18)
    return jnp.clip(entries, -limit, limit).astype(kind)


def setup_inputs(seed: int = 0) -> dict:
    key_list = jax.random.split(jax.random.key(seed), 12)
    stream = scatter_about(key_list[0], (TOKENS, D), 1.0, 6.0, ((0, 32),))
    queries = draw_queries(jax.random.fold_in(key_list[11], 71), 0)
    keys = draw_keys(jax.random.fold_in(key_list[11], 71), 0)
    values = scatter_about(key_list[3], (TOKENS, H * DV), 1.0, 6.0, ((0, 8), (1, 4)))
    head_lambda = jnp.clip(0.3 + 0.5 * jax.random.uniform(key_list[4], (H,), jnp.float32) ** levels(key_list[4], (H,), ((0, 4),), -0.2, 0.2), 0.3, 0.8)
    head_gain = jnp.clip(1.0 + 0.18 * jax.random.normal(key_list[5], (DV,), jnp.float32), 0.1, 1.9)
    w_out = scatter_about(key_list[6], (H * DV, D), (H * DV) ** -0.5, 0.125, ((0, 4),))
    norm_gain = jnp.clip(1.0 + 0.18 * jax.random.normal(key_list[7], (D,), jnp.float32), 0.1, 1.9)
    w_gate = scatter_about(key_list[8], (D, FF), D ** -0.5, 0.125, ((0, 8), (1, 4)))
    w_up = scatter_about(key_list[9], (D, FF), D ** -0.5, 0.125, ((0, 8), (1, 4)))
    w_down = scatter_about(key_list[10], (FF, D), FF ** -0.5, 0.078125, ((0, 4), (1, 8)))
    return {"stream": stream, "queries": queries, "keys": keys, "values": values, "head_lambda": head_lambda, "head_gain": head_gain, "w_out": w_out, "norm_gain": norm_gain, "w_gate": w_gate, "w_up": w_up, "w_down": w_down}


epsilon = 1e-06

def normalize(values_in, gain):
    square_mean = lax.optimization_barrier(jnp.mean(values_in * values_in, axis=-1, keepdims=True))
    return values_in * lax.rsqrt(square_mean + epsilon) * gain

def reference(stream, queries, keys, values, head_lambda, head_gain, w_out, norm_gain, w_gate, w_up, w_down):
    token_count = queries.shape[0]
    query_heads = queries.reshape(token_count, H, 2, DH)
    key_heads = keys.reshape(token_count, H, 2, DH).astype(jnp.float32)
    value_heads = values.reshape(token_count, H, DV).astype(jnp.float32)
    block_rows = math.gcd(token_count, 256)
    key_pos = jnp.arange(token_count, dtype=jnp.int32)
    score_scale = DH ** (-0.5)

    def one_block(block_index):
        query_block = lax.dynamic_slice_in_dim(query_heads, (block_index * block_rows).astype(jnp.int32), block_rows, 0).astype(jnp.float32)
        scores = jnp.einsum('qhsd,khsd->hsqk', query_block, key_heads) * score_scale
        query_pos = block_index * block_rows + jnp.arange(block_rows, dtype=jnp.int32)
        visible = key_pos[None, :] <= query_pos[:, None]
        row_max = lax.optimization_barrier(jnp.max(jnp.where(visible, scores, -1e+30), axis=-1, keepdims=True))
        weights = jnp.where(visible, jnp.exp(scores - row_max), 0.0)
        weight_sum = lax.optimization_barrier(jnp.sum(weights, axis=-1))
        rounded = lax.optimization_barrier(weights.astype(jnp.bfloat16)).astype(jnp.float32)
        map_out = jnp.einsum('hsqk,khd->hsqd', rounded, value_heads) / weight_sum[..., None]
        contrast = map_out[:, 0] - head_lambda[:, None, None] * map_out[:, 1]
        normed_heads = normalize(contrast, head_gain)
        return normed_heads.transpose(1, 0, 2).reshape(block_rows, H * DV).astype(jnp.bfloat16)
    head_out = lax.map(one_block, jnp.arange(token_count // block_rows, dtype=jnp.int32)).reshape(token_count, H * DV)
    middle = stream.astype(jnp.float32) + jnp.dot(head_out, w_out, preferred_element_type=jnp.float32)
    normed = normalize(middle, norm_gain).astype(jnp.bfloat16)
    gate = jnp.dot(normed, w_gate, preferred_element_type=jnp.float32)
    up_part = jnp.dot(normed, w_up, preferred_element_type=jnp.float32)
    hidden = (jax.nn.silu(gate) * up_part).astype(jnp.bfloat16)
    mixed = jnp.dot(hidden, w_down, preferred_element_type=jnp.float32)
    return (middle + mixed).astype(jnp.bfloat16)
```

```python
import functools

import jax
import jax.numpy as jnp
from jax import lax
from jax.experimental import pallas as pl
from jax.experimental.pallas import tpu as pltpu
from jax.sharding import PartitionSpec as P

epsilon = 1e-06
MESH = pl.DeviceIdType.MESH
LANES = 128


def remote(src, dst, send_sem, recv_sem, sp, tp):
    return pltpu.make_async_remote_copy(
        src_ref=src,
        dst_ref=dst,
        send_sem=send_sem,
        recv_sem=recv_sem,
        device_id={"sp": sp, "tp": tp},
        device_id_type=MESH,
    )


def greet(peers):
    barrier = pltpu.get_barrier_semaphore()
    for sp, tp in peers:
        pl.semaphore_signal(
            barrier, inc=1, device_id={"sp": sp, "tp": tp}, device_id_type=MESH
        )
    pl.semaphore_wait(barrier, len(peers))


def when(condition, action):
    if condition is True:
        action()
    elif condition is not False:
        pl.when(condition)(action)


def spread_kernel(
    outer, inner, width,
    k, v, wg, wu, wd,
    kg, vg, gg, ug, dg,
    kv_up, kv_across, w_out_sem, w_across, recv, own_sem,
):
    s, t = lax.axis_index("sp"), lax.axis_index("tp")
    z, i = s // inner, s % inner
    units = wg.shape[1]
    greet(
        [((z + d) % outer * inner + i, t) for d in range(1, outer)]
        + [(z * inner + (i + e) % inner, t) for e in range(1, inner)]
    )

    def start_of(m):
        return pl.multiple_of(jnp.minimum(m * width, units - width), LANES)

    def weights(m):
        cut = pl.ds(start_of(m), width)
        return (wg.at[:, cut], wu.at[:, cut], wd.at[cut, :])

    pairs = ((k, kg), (v, vg))
    slots = (gg, ug, dg)

    def arrived(ref, slot, kind):
        remote(ref.at[slot], ref.at[slot], own_sem.at[0], recv.at[kind, slot], s, t).wait_recv()

    up_copies, across_copies, weight_copies, forward_copies = [], [], [], []
    for a in range(outer):
        slot = (z - a) * inner + i
        for kind, (mine, held) in enumerate(pairs):
            src = mine if a == 0 else held.at[slot]
            up = remote(
                src, held.at[slot], kv_up.at[kind, a], recv.at[kind, slot], s + inner, t
            )
            across = [
                (
                    remote(
                        src, held.at[slot], kv_across.at[kind, a, e], recv.at[kind, slot],
                        z * inner + (i + e) % inner, t,
                    ),
                    ((i + e) % inner > i) if a == 0 else (z >= a),
                )
                for e in range(1, inner)
            ]
            if a > 0:
                pl.when(z >= a)(lambda held=held, slot=slot, kind=kind: arrived(held, slot, kind))
            go_up = jnp.logical_and(z >= a, z + 1 < outer)
            pl.when(go_up)(up.start)
            for copy, needed in across:
                pl.when(needed)(copy.start)
            up_copies.append((up, go_up))
            across_copies += across
        if a == 0:
            own = [
                pltpu.make_async_copy(src, dst.at[s], own_sem.at[n])
                for n, (src, dst) in enumerate(
                    tuple(pairs) + tuple(zip(weights(z), slots))
                )
            ]
            for copy in own:
                copy.start()
            for d in range(1, outer):
                target = (z + d) % outer
                for kind, (src, held) in enumerate(zip(weights(target), slots)):
                    copy = remote(
                        src, held.at[s], w_out_sem.at[kind, d], recv.at[kind + 2, s],
                        target * inner + i, t,
                    )
                    copy.start()
                    weight_copies.append(copy)
        origin = (z + outer - a) % outer * inner + i
        for kind, (src, held) in enumerate(zip(weights(z), slots)):
            if a > 0:
                arrived(held, origin, kind + 2)
                src = held.at[origin]
            for e in range(1, inner):
                copy = remote(
                    src, held.at[origin], w_across.at[kind, a, e], recv.at[kind + 2, origin],
                    z * inner + (i + e) % inner, t,
                )
                copy.start()
                forward_copies.append(copy)
    for e in range(1, inner):
        other = (i + e) % inner
        for a in range(outer):
            slot = (z - a) * inner + other
            for kind, (mine, held) in enumerate(pairs):
                pl.when((other < i) if a == 0 else (z >= a))(
                    lambda held=held, slot=slot, kind=kind: arrived(held, slot, kind)
                )
            for kind, held in enumerate(slots):
                arrived(held, (z + outer - a) % outer * inner + other, kind + 2)
    for copy, needed in up_copies + across_copies:
        pl.when(needed)(copy.wait_send)
    for copy in weight_copies + forward_copies:
        copy.wait_send()
    for copy in own:
        copy.wait()


def spread(keys, values, w_gate, w_up, w_down, count, outer, width):
    inner = count // outer
    rows, units = w_gate.shape
    columns = w_down.shape[1]
    vmem, hbm = pl.BlockSpec(memory_space=pltpu.VMEM), pl.BlockSpec(memory_space=pl.ANY)
    kind = keys.dtype
    return pl.pallas_call(
        functools.partial(spread_kernel, outer, inner, width),
        out_shape=[
            jax.ShapeDtypeStruct((count,) + keys.shape, kind),
            jax.ShapeDtypeStruct((count,) + values.shape, kind),
            jax.ShapeDtypeStruct((count, rows, width), kind),
            jax.ShapeDtypeStruct((count, rows, width), kind),
            jax.ShapeDtypeStruct((count, width, columns), kind),
        ],
        in_specs=[vmem] * 5,
        out_specs=[hbm] * 5,
        scratch_shapes=[
            pltpu.SemaphoreType.DMA((2, outer)),
            pltpu.SemaphoreType.DMA((2, outer, inner)),
            pltpu.SemaphoreType.DMA((3, outer)),
            pltpu.SemaphoreType.DMA((3, outer, inner)),
            pltpu.SemaphoreType.DMA((5, count)),
            pltpu.SemaphoreType.DMA((5,)),
        ],
        compiler_params=pltpu.CompilerParams(collective_id=0, has_side_effects=True),
    )(keys, values, w_gate, w_up, w_down)


def attend_kernel(
    head_count, place, head_lambda, head_gain, q, kg, vg, w_out, out, row_max, weight_sum, acc, heads
):
    rows = q.shape[0]
    head_dim = q.shape[1] // (2 * head_count)
    value_dim = vg.shape[2] // head_count
    scale = head_dim ** (-0.5)
    row_max[...] = jnp.full_like(row_max, -1e30)
    weight_sum[...] = jnp.zeros_like(weight_sum)
    acc[...] = jnp.zeros_like(acc)

    def block(j, diagonal):
        for unit in range(2 * head_count):
            head = unit // 2
            columns = slice(unit * head_dim, (unit + 1) * head_dim)
            scores = (
                lax.dot_general(
                    q[:, columns], kg[j, :, columns], (((1,), (1,)), ((), ())),
                    preferred_element_type=jnp.float32,
                )
                * scale
            )
            if diagonal:
                seen = lax.broadcasted_iota(jnp.int32, scores.shape, 1) <= (
                    lax.broadcasted_iota(jnp.int32, scores.shape, 0)
                )
                scores = jnp.where(seen, scores, -1e30)
            old = row_max[unit]
            new = jnp.maximum(old, jnp.max(scores, axis=-1, keepdims=True))
            weights = jnp.exp(scores - new)
            if diagonal:
                weights = jnp.where(seen, weights, 0.0)
            fade = jnp.exp(old - new)
            row_max[unit] = new
            weight_sum[unit] = fade * weight_sum[unit] + jnp.sum(weights, axis=-1, keepdims=True)
            acc[unit] = fade * acc[unit] + jnp.dot(
                weights.astype(jnp.bfloat16),
                vg[j, :, head * value_dim : (head + 1) * value_dim],
                preferred_element_type=jnp.float32,
            )

    own = place[0]
    block(own, True)
    lax.fori_loop(0, own, lambda j, c: (block(j, False), c)[1], 0)
    for head in range(head_count):
        first = acc[2 * head] / weight_sum[2 * head]
        second = acc[2 * head + 1] / weight_sum[2 * head + 1]
        contrast = first - head_lambda[head] * second
        mean = jnp.mean(contrast * contrast, axis=-1, keepdims=True)
        heads[:, head * value_dim : (head + 1) * value_dim] = (
            contrast * lax.rsqrt(mean + epsilon) * head_gain[...]
        ).astype(jnp.bfloat16)
    out[...] = jnp.dot(heads[...], w_out[...], preferred_element_type=jnp.float32).astype(out.dtype)


def attend(place, head_lambda, head_gain, queries, kg, vg, w_out):
    head_count = head_lambda.shape[0]
    rows = queries.shape[0]
    value_dim = vg.shape[2] // head_count
    vmem, smem = pl.BlockSpec(memory_space=pltpu.VMEM), pl.BlockSpec(memory_space=pltpu.SMEM)
    units = 2 * head_count
    return pl.pallas_call(
        functools.partial(attend_kernel, head_count),
        out_shape=jax.ShapeDtypeStruct((rows, w_out.shape[1]), jnp.bfloat16),
        in_specs=[smem, smem] + [vmem] * 5,
        out_specs=vmem,
        scratch_shapes=[
            pltpu.VMEM((units, rows, 1), jnp.float32),
            pltpu.VMEM((units, rows, 1), jnp.float32),
            pltpu.VMEM((units, rows, value_dim), jnp.float32),
            pltpu.VMEM((rows, vg.shape[2]), jnp.bfloat16),
        ],
    )(place, head_lambda, head_gain.reshape(1, -1), queries, kg, vg, w_out)


def middle_kernel(
    outer, inner, high, low,
    projected, stream, gain, middle, gathered,
    parts, mine, first_send, first_recv, line_send, high_send, low_send, recv, own_sem,
):
    s, t = lax.axis_index("sp"), lax.axis_index("tp")
    z, i = s // inner, s % inner
    hi, lo = t // low, t % low
    tp = high * low
    rows = stream.shape[0]
    greet(
        [(s, (t + d) % tp) for d in range(1, tp)]
        + [((z + d) % outer * inner + i, t) for d in range(1, outer)]
    )
    first = []
    for d in range(1, tp):
        peer = (t + d) % tp
        copy = remote(
            projected.at[pl.ds(pl.multiple_of(peer * rows, rows), rows)], parts.at[t],
            first_send.at[d], first_recv.at[t], s, peer,
        )
        copy.start()
        first.append(copy)
    total = projected[pl.ds(pl.multiple_of(t * rows, rows), rows)].astype(jnp.float32)
    for d in range(1, tp):
        peer = (t + d) % tp
        remote(
            parts.at[peer], parts.at[peer], first_send.at[0], first_recv.at[peer], s, t
        ).wait_recv()
        total = total + parts[peer].astype(jnp.float32)
    total = total + stream[...].astype(jnp.float32)
    middle[...] = total
    mean = jnp.mean(total * total, axis=-1, keepdims=True)
    mine[...] = (total * lax.rsqrt(mean + epsilon) * gain[...]).astype(jnp.bfloat16)

    def arrived(zz, tt):
        remote(
            gathered.at[zz, tt], gathered.at[zz, tt], own_sem, recv.at[zz, tt], s, t
        ).wait_recv()

    copies = []
    for d in range(1, outer):
        copy = remote(
            mine, gathered.at[z, t], line_send.at[d], recv.at[z, t],
            (z + d) % outer * inner + i, t,
        )
        copy.start()
        copies.append(copy)
    own = pltpu.make_async_copy(mine, gathered.at[z, t], own_sem)
    own.start()
    for d in range(outer):
        zz = (z + outer - d) % outer
        if d > 0:
            arrived(zz, t)
        src = mine if d == 0 else gathered.at[zz, t]
        for e in range(1, high):
            copy = remote(
                src, gathered.at[zz, t], high_send.at[d, e], recv.at[zz, t],
                s, (hi + e) % high * low + lo,
            )
            copy.start()
            copies.append(copy)
        for f in range(1, low):
            copy = remote(
                src, gathered.at[zz, t], low_send.at[d, 0, f], recv.at[zz, t],
                s, hi * low + (lo + f) % low,
            )
            copy.start()
            copies.append(copy)
    for d in range(outer):
        zz = (z + outer - d) % outer
        for e in range(1, high):
            tt = (hi + e) % high * low + lo
            arrived(zz, tt)
            for f in range(1, low):
                copy = remote(
                    gathered.at[zz, tt], gathered.at[zz, tt], low_send.at[d, e, f],
                    recv.at[zz, tt], s, hi * low + (lo + f) % low,
                )
                copy.start()
                copies.append(copy)
    for d in range(outer):
        zz = (z + outer - d) % outer
        for e in range(high):
            for f in range(1, low):
                arrived(zz, (hi + e) % high * low + (lo + f) % low)
    for copy in first + copies:
        copy.wait_send()
    own.wait()


def middle_rows(projected, stream, gain, outer, inner, high, low):
    rows, width = stream.shape
    tp = high * low
    vmem = pl.BlockSpec(memory_space=pltpu.VMEM)
    dma = pltpu.SemaphoreType.DMA
    return pl.pallas_call(
        functools.partial(middle_kernel, outer, inner, high, low),
        out_shape=[
            jax.ShapeDtypeStruct((rows, width), jnp.float32),
            jax.ShapeDtypeStruct((outer, tp, rows, width), jnp.bfloat16),
        ],
        in_specs=[vmem] * 3,
        out_specs=[vmem] * 2,
        scratch_shapes=[
            pltpu.VMEM((tp, rows, width), jnp.bfloat16),
            pltpu.VMEM((rows, width), jnp.bfloat16),
            dma((tp,)),
            dma((tp,)),
            dma((outer,)),
            dma((outer, high)),
            dma((outer, high, low)),
            dma((outer, tp)),
            dma,
        ],
        compiler_params=pltpu.CompilerParams(collective_id=1, has_side_effects=True),
    )(projected, stream, gain.reshape(1, -1))


def reduce_kernel(
    outer, inner, high, low,
    partial, middle, out,
    in_low, in_high, in_line, sum_low, sum_high,
    low_send, low_recv, high_send, high_recv, line_send, line_recv,
):
    s, t = lax.axis_index("sp"), lax.axis_index("tp")
    z, i = s // inner, s % inner
    hi, lo = t // low, t % low
    greet(
        [(s, hi * low + (lo + f) % low) for f in range(1, low)]
        + [(s, (hi + e) % high * low + lo) for e in range(1, high)]
        + [((z + d) % outer * inner + i, t) for d in range(1, outer)]
    )
    order = [(z + d) % outer for d in range(1, outer + 1)]
    copies = []
    for d, zz in enumerate(order):
        for e in range(1, high + 1):
            hh = (hi + e) % high
            for f in range(1, low):
                other = (lo + f) % low
                copy = remote(
                    partial.at[zz, hh * low + other], in_low.at[f, zz, hh],
                    low_send.at[f, d, e % high], low_recv.at[f, zz, hh],
                    s, hi * low + other,
                )
                copy.start()
                copies.append(copy)
    for d, zz in enumerate(order):
        for e in range(1, high + 1):
            hh = (hi + e) % high
            total = partial[zz, hh * low + lo].astype(jnp.float32)
            for f in range(1, low):
                remote(
                    in_low.at[f, zz, hh], in_low.at[f, zz, hh], low_send.at[f, d, e % high],
                    low_recv.at[f, zz, hh], s, t,
                ).wait_recv()
                total = total + in_low[f, zz, hh].astype(jnp.float32)
            sum_low[zz, hh] = total.astype(jnp.bfloat16)
            if e < high:
                copy = remote(
                    sum_low.at[zz, hh], in_high.at[e, zz], high_send.at[e, d],
                    high_recv.at[e, zz], s, hh * low + lo,
                )
                copy.start()
                copies.append(copy)
    for d, zz in enumerate(order):
        total = sum_low[zz, hi].astype(jnp.float32)
        for e in range(1, high):
            remote(
                in_high.at[e, zz], in_high.at[e, zz], high_send.at[e, d],
                high_recv.at[e, zz], s, t,
            ).wait_recv()
            total = total + in_high[e, zz].astype(jnp.float32)
        if d + 1 < outer:
            sum_high[d] = total.astype(jnp.bfloat16)
            copy = remote(
                sum_high.at[d], in_line.at[d], line_send.at[d], line_recv.at[d],
                zz * inner + i, t,
            )
            copy.start()
            copies.append(copy)
    total = total + middle[...]
    for d in range(outer - 1):
        remote(
            in_line.at[d], in_line.at[d], line_send.at[d], line_recv.at[d], s, t
        ).wait_recv()
        total = total + in_line[d].astype(jnp.float32)
    out[...] = total.astype(out.dtype)
    for copy in copies:
        copy.wait_send()


def reduce_rows(partial, middle, outer, inner, high, low):
    rows, width = middle.shape
    vmem = pl.BlockSpec(memory_space=pltpu.VMEM)
    dma = pltpu.SemaphoreType.DMA
    kind = jnp.bfloat16
    return pl.pallas_call(
        functools.partial(reduce_kernel, outer, inner, high, low),
        out_shape=jax.ShapeDtypeStruct((rows, width), kind),
        in_specs=[vmem] * 2,
        out_specs=vmem,
        scratch_shapes=[
            pltpu.VMEM((low, outer, high, rows, width), kind),
            pltpu.VMEM((high, outer, rows, width), kind),
            pltpu.VMEM((outer, rows, width), kind),
            pltpu.VMEM((outer, high, rows, width), kind),
            pltpu.VMEM((outer, rows, width), kind),
            dma((low, outer, high)),
            dma((low, outer, high)),
            dma((high, outer)),
            dma((high, outer)),
            dma((outer,)),
            dma((outer,)),
        ],
        compiler_params=pltpu.CompilerParams(collective_id=2, has_side_effects=True),
    )(partial, middle)


def largest_part(count, limit):
    return max(part for part in range(1, limit + 1) if count % part == 0)


def shards(
    count, tp,
    stream, queries, keys, values, head_lambda, head_gain, w_out, norm_gain, w_gate, w_up, w_down,
):
    outer = largest_part(count, 4)
    inner = count // outer
    low = largest_part(tp, 2)
    high = tp // low
    units = w_gate.shape[1]
    width = -(-units // (LANES * outer)) * LANES
    rows, model = stream.shape
    s = lax.axis_index("sp")
    place = s.astype(jnp.int32).reshape(1)
    kg, vg, gg, ug, dg = spread(keys, values, w_gate, w_up, w_down, count, outer, width)
    projected = attend(place, head_lambda, head_gain, queries, kg, vg, w_out)
    middle, gathered = middle_rows(projected, stream, norm_gain, outer, inner, high, low)
    normed = gathered.reshape(-1, model)
    gate = jnp.dot(normed, gg.reshape(-1, width), preferred_element_type=jnp.float32)
    up_part = jnp.dot(normed, ug.reshape(-1, width), preferred_element_type=jnp.float32)
    hidden = (jax.nn.silu(gate) * up_part).astype(jnp.bfloat16)
    begin = (s // inner) * width
    repeated = begin - jnp.minimum(begin, units - width)
    hidden = jnp.where(jnp.arange(width)[None, :] >= repeated, hidden, 0).astype(jnp.bfloat16)
    down = dg.transpose(1, 0, 2).reshape(width, -1)
    partial = jnp.dot(hidden, down, preferred_element_type=jnp.float32).astype(jnp.bfloat16)
    return reduce_rows(
        partial.reshape(outer, tp, rows, model), middle, outer, inner, high, low
    )


def solution(mesh):
    placed = (
        P(("sp", "tp"), None),
        P("sp", "tp"),
        P("sp", "tp"),
        P("sp", "tp"),
        P("tp"),
        P(),
        P("tp", None),
        P(),
        P("sp", "tp"),
        P("sp", "tp"),
        P("tp", "sp"),
    )
    return jax.shard_map(
        functools.partial(shards, mesh.shape["sp"], mesh.shape["tp"]),
        mesh=mesh,
        in_specs=placed,
        out_specs=P(("sp", "tp"), None),
        check_vma=False,
    )
```

```python
import functools

import jax
import jax.numpy as jnp
from jax import lax
from jax.experimental import pallas as pl
from jax.experimental.pallas import tpu as pltpu
from jax.sharding import PartitionSpec as P

epsilon = 1e-06
MESH = pl.DeviceIdType.MESH
LANES = 128


def remote(src, dst, send_sem, recv_sem, sp, tp):
    return pltpu.make_async_remote_copy(
        src_ref=src,
        dst_ref=dst,
        send_sem=send_sem,
        recv_sem=recv_sem,
        device_id={"sp": sp, "tp": tp},
        device_id_type=MESH,
    )


def greet(peers):
    barrier = pltpu.get_barrier_semaphore()
    for sp, tp in peers:
        pl.semaphore_signal(
            barrier, inc=1, device_id={"sp": sp, "tp": tp}, device_id_type=MESH
        )
    pl.semaphore_wait(barrier, len(peers))


def when(condition, action):
    if condition is True:
        action()
    elif condition is not False:
        pl.when(condition)(action)


def front_kernel(
    outer, inner, high, low, width, head_count,
    head_lambda, head_gain, stream, q, k, v, w_out, gain, wg, wu, wd,
    middle, gathered, gg, ug, dg,
    kg, vg, row_max, weight_sum, acc, heads, projected, parts, mine,
    kv_up, kv_across, kv_recv, w_send, w_across, w_recv, own_sem,
    first_send, first_recv, line_send, high_send, low_send, recv,
):
    s, t = lax.axis_index("sp"), lax.axis_index("tp")
    z, i = s // inner, s % inner
    hi, lo = t // low, t % low
    tp = high * low
    units = wg.shape[1]
    rows = stream.shape[0]
    head_dim = q.shape[1] // (2 * head_count)
    value_dim = v.shape[1] // head_count
    scale = head_dim ** (-0.5)
    greet(
        [((z + d) % outer * inner + i, t) for d in range(1, outer)]
        + [(z * inner + (i + e) % inner, t) for e in range(1, inner)]
        + [(s, (t + d) % tp) for d in range(1, tp)]
    )

    def start_of(m):
        return pl.multiple_of(jnp.minimum(m * width, units - width), LANES)

    def weights(m):
        cut = pl.ds(start_of(m), width)
        return (wg.at[:, cut], wu.at[:, cut], wd.at[cut, :])

    pairs = ((k, kg), (v, vg))
    slots = (gg, ug, dg)
    sent = []

    def kv_arrived(slot):
        for kind, (mine_, held) in enumerate(pairs):
            remote(
                held.at[slot], held.at[slot], kv_up.at[0, 0], kv_recv.at[kind, slot], s, t
            ).wait_recv()

    def weights_arrived(slot):
        for kind, held in enumerate(slots):
            remote(
                held.at[slot], held.at[slot], w_send.at[0, 0], w_recv.at[kind, slot], s, t
            ).wait_recv()

    def send(copy, needed):
        if needed is True:
            copy.start()
        else:
            pl.when(needed)(copy.start)
        sent.append((copy, needed))

    def pass_kv(a):
        slot = (z - a) * inner + i
        for kind, (own_block, held) in enumerate(pairs):
            src = own_block if a == 0 else held.at[slot]
            send(
                remote(src, held.at[slot], kv_up.at[kind, a], kv_recv.at[kind, slot], s + inner, t),
                jnp.logical_and(z >= a, z + 1 < outer),
            )
            for e in range(1, inner):
                other = (i + e) % inner
                send(
                    remote(
                        src, held.at[slot], kv_across.at[kind, a, e], kv_recv.at[kind, slot],
                        z * inner + other, t,
                    ),
                    (other > i) if a == 0 else (z >= a),
                )

    def send_weights(offset):
        target = z + offset
        for kind, (src, held) in enumerate(zip(weights(target), slots)):
            send(
                remote(
                    src, held.at[s], w_send.at[kind, outer + offset], w_recv.at[kind, s],
                    target * inner + i, t,
                ),
                (target >= 0) if offset < 0 else (target < outer),
            )

    def forward_weights(offset):
        origin = (z + offset) * inner + i
        needed = True
        if offset:
            needed = (z + offset >= 0) if offset < 0 else (z + offset < outer)
            pl.when(needed)(lambda: weights_arrived(origin))
        for kind, (src, held) in enumerate(zip(weights(z), slots)):
            for e in range(1, inner):
                send(
                    remote(
                        held.at[origin] if offset else src, held.at[origin],
                        w_across.at[kind, outer + offset, e], w_recv.at[kind, origin],
                        z * inner + (i + e) % inner, t,
                    ),
                    needed,
                )

    def block(k_block, v_block, diagonal):
        for unit in range(2 * head_count):
            head = unit // 2
            columns = slice(unit * head_dim, (unit + 1) * head_dim)
            scores = (
                lax.dot_general(
                    q[:, columns], k_block[:, columns], (((1,), (1,)), ((), ())),
                    preferred_element_type=jnp.float32,
                )
                * scale
            )
            if diagonal:
                seen = lax.broadcasted_iota(jnp.int32, scores.shape, 1) <= (
                    lax.broadcasted_iota(jnp.int32, scores.shape, 0)
                )
                scores = jnp.where(seen, scores, -1e30)
            top = jnp.max(scores, axis=-1, keepdims=True)
            new = top if diagonal else jnp.maximum(row_max[unit], top)
            weights_ = jnp.exp(scores - new)
            if diagonal:
                weights_ = jnp.where(seen, weights_, 0.0)
            total = jnp.sum(weights_, axis=-1, keepdims=True)
            added = jnp.dot(
                weights_.astype(jnp.bfloat16),
                v_block[:, head * value_dim : (head + 1) * value_dim],
                preferred_element_type=jnp.float32,
            )
            if diagonal:
                weight_sum[unit] = total
                acc[unit] = added
            else:
                fade = jnp.exp(row_max[unit] - new)
                weight_sum[unit] = fade * weight_sum[unit] + total
                acc[unit] = fade * acc[unit] + added
            row_max[unit] = new

    pass_kv(0)
    own = [
        pltpu.make_async_copy(src, dst.at[s], own_sem.at[n])
        for n, (src, dst) in enumerate(zip(weights(z), slots))
    ]
    for copy in own:
        copy.start()
    for d in range(1, outer):
        send_weights(-d)
    forward_weights(0)
    block(k, v, True)
    for a in range(1, outer):
        slot = (z - a) * inner + i
        pl.when(z >= a)(lambda slot=slot: kv_arrived(slot))
        pass_kv(a)
        pl.when(z >= a)(lambda slot=slot: block(kg.at[slot], vg.at[slot], False))
    for d in range(1, outer):
        send_weights(d)
    for a in range(outer):
        for e in range(1, inner):
            other = (i + e) % inner
            slot = (z - a) * inner + other

            def take(slot=slot):
                kv_arrived(slot)
                block(kg.at[slot], vg.at[slot], False)

            pl.when((other < i) if a == 0 else (z >= a))(take)
    for head in range(head_count):
        contrast = (
            acc[2 * head] / weight_sum[2 * head]
            - head_lambda[head] * (acc[2 * head + 1] / weight_sum[2 * head + 1])
        )
        mean = jnp.mean(contrast * contrast, axis=-1, keepdims=True)
        heads[:, head * value_dim : (head + 1) * value_dim] = (
            contrast * lax.rsqrt(mean + epsilon) * head_gain[...]
        ).astype(jnp.bfloat16)
    projected[...] = jnp.dot(
        heads[...], w_out[...], preferred_element_type=jnp.float32
    ).astype(projected.dtype)

    for d in range(1, tp):
        peer = (t + d) % tp
        send(
            remote(
                projected.at[pl.ds(pl.multiple_of(peer * rows, rows), rows)], parts.at[t],
                first_send.at[d], first_recv.at[t], s, peer,
            ),
            True,
        )
    for d in range(1, outer):
        forward_weights(d)
    total = projected[pl.ds(pl.multiple_of(t * rows, rows), rows)].astype(jnp.float32)
    for d in range(1, tp):
        peer = (t + d) % tp
        remote(
            parts.at[peer], parts.at[peer], first_send.at[0], first_recv.at[peer], s, t
        ).wait_recv()
        total = total + parts[peer].astype(jnp.float32)
    total = total + stream[...].astype(jnp.float32)
    middle[...] = total
    mean = jnp.mean(total * total, axis=-1, keepdims=True)
    mine[...] = (total * lax.rsqrt(mean + epsilon) * gain[...]).astype(jnp.bfloat16)

    def arrived(zz, tt):
        remote(
            gathered.at[zz, tt], gathered.at[zz, tt], first_send.at[0], recv.at[zz, tt], s, t
        ).wait_recv()

    def pass_rows(d):
        zz = (z + outer - d) % outer
        src = mine if d == 0 else gathered.at[zz, t]
        for e in range(1, high):
            send(
                remote(
                    src, gathered.at[zz, t], high_send.at[d, e], recv.at[zz, t],
                    s, (hi + e) % high * low + lo,
                ),
                True,
            )
        for f in range(1, low):
            send(
                remote(
                    src, gathered.at[zz, t], low_send.at[d, 0, f], recv.at[zz, t],
                    s, hi * low + (lo + f) % low,
                ),
                True,
            )

    for d in range(1, outer):
        send(
            remote(
                mine, gathered.at[z, t], line_send.at[d], recv.at[z, t],
                (z + d) % outer * inner + i, t,
            ),
            True,
        )
    own_rows = pltpu.make_async_copy(mine, gathered.at[z, t], own_sem.at[3])
    own_rows.start()
    pass_rows(0)
    for d in range(1, outer):
        forward_weights(-d)
    for d in range(1, outer):
        arrived((z + outer - d) % outer, t)
        pass_rows(d)
    for d in range(outer):
        zz = (z + outer - d) % outer
        for e in range(1, high):
            tt = (hi + e) % high * low + lo
            arrived(zz, tt)
            for f in range(1, low):
                send(
                    remote(
                        gathered.at[zz, tt], gathered.at[zz, tt], low_send.at[d, e, f],
                        recv.at[zz, tt], s, hi * low + (lo + f) % low,
                    ),
                    True,
                )
    for d in range(outer):
        for e in range(high):
            for f in range(1, low):
                arrived((z + outer - d) % outer, (hi + e) % high * low + (lo + f) % low)
    for e in range(1, inner):
        for a in range(outer):
            weights_arrived((z + outer - a) % outer * inner + (i + e) % inner)
    for copy, needed in sent:
        if needed is True:
            copy.wait_send()
        else:
            pl.when(needed)(copy.wait_send)
    for copy in own + [own_rows]:
        copy.wait()


def front(
    stream, queries, keys, values, head_lambda, head_gain, w_out, norm_gain, w_gate, w_up, w_down,
    outer, inner, high, low, width,
):
    count, tp = outer * inner, high * low
    depth = w_gate.shape[0]
    columns = w_down.shape[1]
    rows, model = stream.shape
    tokens = queries.shape[0]
    head_count = head_lambda.shape[0]
    value_dim = values.shape[1] // head_count
    vmem, hbm = pl.BlockSpec(memory_space=pltpu.VMEM), pl.BlockSpec(memory_space=pl.ANY)
    smem = pl.BlockSpec(memory_space=pltpu.SMEM)
    dma = pltpu.SemaphoreType.DMA
    kind = jnp.bfloat16
    return pl.pallas_call(
        functools.partial(front_kernel, outer, inner, high, low, width, head_count),
        out_shape=[
            jax.ShapeDtypeStruct((rows, model), jnp.float32),
            jax.ShapeDtypeStruct((outer, tp, rows, model), kind),
            jax.ShapeDtypeStruct((count, depth, width), kind),
            jax.ShapeDtypeStruct((count, depth, width), kind),
            jax.ShapeDtypeStruct((count, width, columns), kind),
        ],
        in_specs=[smem] + [vmem] * 10,
        out_specs=[vmem, vmem, hbm, hbm, hbm],
        scratch_shapes=[
            pltpu.VMEM((count,) + keys.shape, kind),
            pltpu.VMEM((count,) + values.shape, kind),
            pltpu.VMEM((2 * head_count, tokens, 1), jnp.float32),
            pltpu.VMEM((2 * head_count, tokens, 1), jnp.float32),
            pltpu.VMEM((2 * head_count, tokens, value_dim), jnp.float32),
            pltpu.VMEM((tokens, values.shape[1]), kind),
            pltpu.VMEM((tokens, model), kind),
            pltpu.VMEM((tp, rows, model), kind),
            pltpu.VMEM((rows, model), kind),
            dma((2, outer)),
            dma((2, outer, inner)),
            dma((2, count)),
            dma((3, 2 * outer)),
            dma((3, 2 * outer, inner)),
            dma((3, count)),
            dma((4,)),
            dma((tp,)),
            dma((tp,)),
            dma((outer,)),
            dma((outer, high)),
            dma((outer, high, low)),
            dma((outer, tp)),
        ],
        compiler_params=pltpu.CompilerParams(collective_id=0, has_side_effects=True),
    )(
        head_lambda, head_gain.reshape(1, -1), stream, queries, keys, values, w_out,
        norm_gain.reshape(1, -1), w_gate, w_up, w_down,
    )


def back_kernel(
    outer, inner, high, low, units,
    normed, wg, wu, wd, middle, out,
    partial, in_low, in_high, in_line, sum_low, sum_high,
    low_send, low_recv, high_send, high_recv, line_send, line_recv,
):
    s, t = lax.axis_index("sp"), lax.axis_index("tp")
    z, i = s // inner, s % inner
    hi, lo = t // low, t % low
    tp = high * low
    rows, model = middle.shape
    width = wg.shape[1]
    greet(
        [(s, hi * low + (lo + f) % low) for f in range(1, low)]
        + [(s, (hi + e) % high * low + lo) for e in range(1, high)]
        + [((z + d) % outer * inner + i, t) for d in range(1, outer)]
    )
    repeated = z * width - jnp.minimum(z * width, units - width)
    copies = []

    def start(copy):
        copy.start()
        copies.append(copy)

    def compute(d):
        zz = (z + d + 1) % outer
        chunk = normed[zz].reshape(tp * rows, model)
        gate = jnp.dot(chunk, wg[...], preferred_element_type=jnp.float32)
        up_part = jnp.dot(chunk, wu[...], preferred_element_type=jnp.float32)
        hidden = gate / (1.0 + jnp.exp(-gate)) * up_part
        mine = lax.broadcasted_iota(jnp.int32, hidden.shape, 1) >= repeated
        hidden = jnp.where(mine, hidden, 0.0).astype(jnp.bfloat16)
        partial[zz] = (
            jnp.dot(hidden, wd[...], preferred_element_type=jnp.float32)
            .astype(partial.dtype)
            .reshape(tp, rows, model)
        )
        for e in range(1, high + 1):
            hh = (hi + e) % high
            for f in range(1, low):
                other = (lo + f) % low
                start(
                    remote(
                        partial.at[zz, hh * low + other], in_low.at[f, zz, hh],
                        low_send.at[f, d, e % high], low_recv.at[f, zz, hh],
                        s, hi * low + other,
                    )
                )

    def add_low(d):
        zz = (z + d + 1) % outer
        for e in range(1, high + 1):
            hh = (hi + e) % high
            total = partial[zz, hh * low + lo].astype(jnp.float32)
            for f in range(1, low):
                remote(
                    in_low.at[f, zz, hh], in_low.at[f, zz, hh], low_send.at[f, d, e % high],
                    low_recv.at[f, zz, hh], s, t,
                ).wait_recv()
                total = total + in_low[f, zz, hh].astype(jnp.float32)
            sum_low[zz, hh] = total.astype(jnp.bfloat16)
            if e < high:
                start(
                    remote(
                        sum_low.at[zz, hh], in_high.at[e, zz], high_send.at[e, d],
                        high_recv.at[e, zz], s, hh * low + lo,
                    )
                )

    def add_high(d):
        zz = (z + d + 1) % outer
        total = sum_low[zz, hi].astype(jnp.float32)
        for e in range(1, high):
            remote(
                in_high.at[e, zz], in_high.at[e, zz], high_send.at[e, d],
                high_recv.at[e, zz], s, t,
            ).wait_recv()
            total = total + in_high[e, zz].astype(jnp.float32)
        if d + 1 < outer:
            sum_high[d] = total.astype(jnp.bfloat16)
            start(
                remote(
                    sum_high.at[d], in_line.at[d], line_send.at[d], line_recv.at[d],
                    zz * inner + i, t,
                )
            )
        return total

    for step in range(outer + 2):
        if step < outer:
            compute(step)
        if 0 <= step - 1 < outer:
            add_low(step - 1)
        if 0 <= step - 2 < outer:
            total = add_high(step - 2)
    total = total + middle[...]
    for d in range(outer - 1):
        remote(
            in_line.at[d], in_line.at[d], line_send.at[d], line_recv.at[d], s, t
        ).wait_recv()
        total = total + in_line[d].astype(jnp.float32)
    out[...] = total.astype(out.dtype)
    for copy in copies:
        copy.wait_send()


def back(gathered, w_gate, w_up, w_down, middle, outer, inner, high, low, units):
    rows, width = middle.shape
    vmem = pl.BlockSpec(memory_space=pltpu.VMEM)
    dma = pltpu.SemaphoreType.DMA
    kind = jnp.bfloat16
    return pl.pallas_call(
        functools.partial(back_kernel, outer, inner, high, low, units),
        out_shape=jax.ShapeDtypeStruct((rows, width), kind),
        in_specs=[vmem] * 5,
        out_specs=vmem,
        scratch_shapes=[
            pltpu.VMEM((outer, high * low, rows, width), kind),
            pltpu.VMEM((low, outer, high, rows, width), kind),
            pltpu.VMEM((high, outer, rows, width), kind),
            pltpu.VMEM((outer, rows, width), kind),
            pltpu.VMEM((outer, high, rows, width), kind),
            pltpu.VMEM((outer, rows, width), kind),
            dma((low, outer, high)),
            dma((low, outer, high)),
            dma((high, outer)),
            dma((high, outer)),
            dma((outer,)),
            dma((outer,)),
        ],
        compiler_params=pltpu.CompilerParams(collective_id=2, has_side_effects=True),
    )(gathered, w_gate, w_up, w_down, middle)


def largest_part(count, limit):
    return max(part for part in range(1, limit + 1) if count % part == 0)


def shards(
    count, tp,
    stream, queries, keys, values, head_lambda, head_gain, w_out, norm_gain, w_gate, w_up, w_down,
):
    outer = largest_part(count, 4)
    inner = count // outer
    low = largest_part(tp, 2)
    high = tp // low
    units = w_gate.shape[1]
    width = -(-units // (LANES * outer)) * LANES
    middle, gathered, gg, ug, dg = front(
        stream, queries, keys, values, head_lambda, head_gain, w_out, norm_gain,
        w_gate, w_up, w_down, outer, inner, high, low, width,
    )
    down = dg.transpose(1, 0, 2).reshape(width, -1)
    return back(
        gathered, gg.reshape(-1, width), ug.reshape(-1, width), down, middle,
        outer, inner, high, low, units,
    )


def solution(mesh):
    placed = (
        P(("sp", "tp"), None),
        P("sp", "tp"),
        P("sp", "tp"),
        P("sp", "tp"),
        P("tp"),
        P(),
        P("tp", None),
        P(),
        P("sp", "tp"),
        P("sp", "tp"),
        P("tp", "sp"),
    )
    return jax.shard_map(
        functools.partial(shards, mesh.shape["sp"], mesh.shape["tp"]),
        mesh=mesh,
        in_specs=placed,
        out_specs=P(("sp", "tp"), None),
        check_vma=False,
    )
```
